768 devices in a mesh: sp: 96 (over z, y), tp: 8 (over x, core).
Axes of the slice: x: 4, y: 8, z: 12, core: 2. Of those that a mesh axis runs over, the one named last changes fastest.
Arguments:
- target: bfloat16 [12288, 2048], P('sp'), may hold values from -160 to 160
- source: bfloat16 [24576, 2048], P(('sp', 'tp')), may hold values from -160 to 160
- query_gain: float32 [2048], replicated, may hold values from 0.1 to 1.9
- source_gain: float32 [2048], replicated, may hold values from 0.1 to 1.9
- query_weight: bfloat16 [2048, 2048], P(None, 'tp'), may hold values from -4 to 4
- key_weight: bfloat16 [2048, 512], replicated, may hold values from -4 to 4
- value_weight: bfloat16 [2048, 512], replicated, may hold values from -1 to 1
- out_weight: bfloat16 [2048, 2048], P('tp'), may hold values from -0.125 to 0.125
- mixer_gain: float32 [2048], replicated, may hold values from 0.1 to 1.9
- gate_weight: bfloat16 [2048, 3072], P(None, 'tp'), may hold values from -0.125 to 0.125
- up_weight: bfloat16 [2048, 3072], P(None, 'tp'), may hold values from -0.125 to 0.125
- gate_taps: bfloat16 [3, 3072], P(None, 'tp'), may hold values from -3.5 to 3.5
- up_taps: bfloat16 [3, 3072], P(None, 'tp'), may hold values from -3.5 to 3.5
- down_weight: bfloat16 [3072, 2048], P('tp'), may hold values from -0.109375 to 0.109375
- final_gain: float32 [2048], replicated, may hold values from 0.1 to 1.9
Outputs:
- layer_out: bfloat16 [12288, 2048], P(('sp', 'tp'))
The draws below stay inside these ranges and needn't reach their ends.
All inputs are finite; a program needn't handle non-finite values.
Results may differ from the reference program's by a relative error of at most 0.012.
Values may be sent and summed in bfloat16 or wider, within the bound.
No kernel may reach another device: no remote copies, remote signals or barrier semaphores. Data moves between devices by JAX's collectives and lax.ppermute only.
A program may use at most 64 MiB of HBM per device.

```python
import math
import jax
import jax.numpy as jnp
from jax import lax

D = 2048
HEADS = 8
HEAD = 256
KV_HEADS = 2
FF = 3072
CONV = 3
TGT_DEV = 128
SRC_DEV = 256
TGT = 12288
SRC = 24576
N_SP = 96
N_TP = 8


def draw_target(key, part):
    result = jax.random.truncated_normal(jax.random.fold_in(key, 11), -4.0, 4.0, (TGT, D), jnp.float32)
    return result.astype(jnp.bfloat16)


def draw_source(key, part):
    result = jax.random.truncated_normal(jax.random.fold_in(key, 31), -4.0, 4.0, (SRC, D), jnp.float32)
    return result.astype(jnp.bfloat16)


def drawn_weight(key, salt, columns):
    drawn = jax.random.truncated_normal(jax.random.fold_in(key, salt), -4.0, 4.0, (D, columns), jnp.float32)
    drawn = drawn * math.sqrt(2.5 / D)
    return drawn.astype(jnp.bfloat16)


def draw_query_weight(key, part):
    return drawn_weight(key, 21, HEADS * HEAD)


def draw_key_weight(key, part):
    return drawn_weight(key, 22, KV_HEADS * HEAD)


def block_scale(own_key, dims, shards, low, top_value):
    level, own = 1.0, jax.random.fold_in(own_key, 6)
    for axis_at, blocks in shards:
        heights = jnp.exp(jax.random.uniform(jax.random.fold_in(own, axis_at), (blocks,), jnp.float32, low / len(shards), top_value / len(shards)))
        level = level * jnp.repeat(heights, dims[axis_at] // blocks).reshape([-1 if axis == axis_at else 1 for axis in range(len(dims))])
    return level


def noise(key, dims, spread, reach, split=(), dtype=jnp.bfloat16):
    entries = spread * jax.random.normal(key, dims, jnp.float32)
    if split:
        entries = entries * block_scale(key, dims, split, -0.22, 0.18)
    return jnp.clip(entries, -reach, reach).astype(dtype)


def setup_inputs(seed: int = 0) -> dict:
    key_of = jax.random.split(jax.random.key(seed), 16)
    target = draw_target(jax.random.fold_in(key_of[15], 71), 0)
    source = draw_source(jax.random.fold_in(key_of[15], 71), 0)
    query_gain = jnp.clip(1.0 + 0.18 * jax.random.normal(key_of[2], (D,), jnp.float32), 0.1, 1.9)
    source_gain = jnp.clip(1.0 + 0.18 * jax.random.normal(key_of[3], (D,), jnp.float32), 0.1, 1.9)
    query_weight = draw_query_weight(jax.random.fold_in(key_of[15], 71), 0)
    key_weight = draw_key_weight(jax.random.fold_in(key_of[15], 71), 0)
    value_weight = noise(key_of[6], (D, KV_HEADS * HEAD), (D // 48) ** -0.5, 1.0)
    out_weight = noise(key_of[7], (HEADS * HEAD, D), (HEADS * HEAD) ** -0.5, 0.125, ((0, 8),))
    mixer_gain = jnp.clip(1.0 + 0.18 * jax.random.normal(key_of[8], (D,), jnp.float32), 0.1, 1.9)
    gate_weight = noise(key_of[9], (D, FF), D ** -0.5, 0.125, ((1, 8),))
    up_weight = noise(key_of[10], (D, FF), D ** -0.5, 0.125, ((1, 8),))
    gate_taps = noise(key_of[11], (CONV, FF), CONV ** -0.5, 3.5, ((1, 8),))
    up_taps = noise(key_of[12], (CONV, FF), CONV ** -0.5, 3.5, ((1, 8),))
    down_weight = noise(key_of[13], (FF, D), FF ** -0.5, 0.109375, ((0, 8),))
    final_gain = jnp.clip(1.0 + 0.18 * jax.random.normal(key_of[14], (D,), jnp.float32), 0.1, 1.9)
    return {"target": target, "source": source, "query_gain": query_gain, "source_gain": source_gain, "query_weight": query_weight, "key_weight": key_weight, "value_weight": value_weight, "out_weight": out_weight, "mixer_gain": mixer_gain, "gate_weight": gate_weight, "up_weight": up_weight, "gate_taps": gate_taps, "up_taps": up_taps, "down_weight": down_weight, "final_gain": final_gain}


EPS = 1e-06

def normalize(values, gain):
    widened = values.astype(jnp.float32)
    scaled = widened * lax.rsqrt(lax.optimization_barrier(jnp.mean(widened * widened, axis=-1, keepdims=True)) + EPS)
    return (scaled * gain.astype(jnp.float32)).astype(jnp.bfloat16)

def rounded(values):
    return lax.optimization_barrier(values.astype(jnp.bfloat16)).astype(jnp.float32)

def reference(target, source, query_gain, source_gain, query_weight, key_weight, value_weight, out_weight, mixer_gain, gate_weight, up_weight, gate_taps, up_taps, down_weight, final_gain):
    group_size = HEADS // KV_HEADS
    slice_rows = SRC_DEV // N_TP
    normed = normalize(target, query_gain)
    queries = rounded(jnp.dot(normed, query_weight, preferred_element_type=jnp.float32))
    source_normed = normalize(source, source_gain)
    key_rows = rounded(jnp.dot(source_normed, key_weight, preferred_element_type=jnp.float32))
    value_rows = rounded(jnp.dot(source_normed, value_weight, preferred_element_type=jnp.float32))
    key_slices = key_rows.reshape(N_SP, N_TP, slice_rows, KV_HEADS, HEAD)
    value_slices = value_rows.reshape(N_SP, N_TP, slice_rows, KV_HEADS, HEAD)
    query_blocks = queries.reshape(N_SP, TGT_DEV, KV_HEADS, group_size, HEAD)
    score_scale = HEAD ** (-0.5)

    def attend(query_block):
        maxima = []
        sums = []
        partial_sums = []
        for slot in range(N_TP):
            slot_keys = key_slices[:, slot].reshape(N_SP * slice_rows, KV_HEADS, HEAD)
            slot_values = value_slices[:, slot].reshape(N_SP * slice_rows, KV_HEADS, HEAD)
            scores = jnp.einsum('bgjd,ngd->gjbn', query_block, slot_keys) * score_scale
            highest = lax.optimization_barrier(jnp.max(scores, axis=-1))
            weights = jnp.exp(scores - highest[..., None])
            maxima.append(highest)
            sums.append(lax.optimization_barrier(jnp.sum(weights, axis=-1)))
            partial_sums.append(jnp.einsum('gjbn,ngd->gjbd', rounded(weights), slot_values))
        maxima = jnp.stack(maxima)
        sums = jnp.stack(sums)
        partial_sums = jnp.stack(partial_sums)
        overall = lax.optimization_barrier(jnp.max(maxima, axis=0))
        factor = jnp.exp(maxima - overall)
        denominator = lax.optimization_barrier(jnp.sum(factor * sums, axis=0))
        merged = lax.optimization_barrier(jnp.sum(factor[..., None] * partial_sums, axis=0)) / denominator[..., None]
        return merged.transpose(2, 0, 1, 3).reshape(TGT_DEV, HEADS * HEAD).astype(jnp.bfloat16)
    attended = lax.map(attend, query_blocks).reshape(N_SP * TGT_DEV, HEADS * HEAD)
    projected = jnp.dot(attended, out_weight, preferred_element_type=jnp.float32)
    residual = (target.astype(jnp.float32) + projected).astype(jnp.bfloat16)
    mixer_in = normalize(residual, mixer_gain)
    gate_rows = rounded(jnp.dot(mixer_in, gate_weight, preferred_element_type=jnp.float32))
    up_rows = rounded(jnp.dot(mixer_in, up_weight, preferred_element_type=jnp.float32))
    stacked = jnp.stack([gate_rows, up_rows])
    padded = jnp.pad(stacked, ((0, 0), (CONV - 1, 0), (0, 0)))
    conv_taps = jnp.stack([gate_taps, up_taps]).astype(jnp.float32)
    total_rows = N_SP * TGT_DEV
    mixed = conv_taps[:, 0:1, :] * padded[:, 0:total_rows, :]
    for index_tap in range(1, CONV):
        mixed = mixed + conv_taps[:, index_tap:index_tap + 1, :] * padded[:, index_tap:index_tap + total_rows, :]
    hidden = (jax.nn.silu(mixed[0]) * mixed[1]).astype(jnp.bfloat16)
    mixer = jnp.dot(hidden, down_weight, preferred_element_type=jnp.float32)
    return normalize(residual.astype(jnp.float32) + mixer, final_gain)
```

```python
import functools

import jax
import jax.numpy as jnp
from jax import lax
from jax.experimental import pallas as pl
from jax.experimental.pallas import tpu as pltpu
from jax.sharding import Mesh
from jax.sharding import PartitionSpec as P

D = 2048
HEADS = 8
HEAD = 256
KV_HEADS = 2
CONV = 3
TGT_DEV = 128
PAD = 16
EPS = 1e-06

M = 2
SP = ("z", "q", "m")
TP = ("g", "xp", "c")
CHIPS = ("g", "xp")
SLICES = ("m", "xp", "c")
BLOCK = 16
HALF = TGT_DEV // 2
bf16 = jnp.bfloat16
f32 = jnp.float32


def normalize(values, gain):
    widened = values.astype(f32)
    scaled = widened * lax.rsqrt(jnp.mean(widened * widened, axis=-1, keepdims=True) + EPS)
    return (scaled * gain).astype(bf16)


def attend_body(q_ref, kv_ref, o_ref):
    k = kv_ref[:, :HEAD]
    v = kv_ref[:, HEAD:]
    row = lax.broadcasted_iota(jnp.int32, (PAD, HEAD), 0)
    for pair in range(0, q_ref.shape[0], 2):
        q = q_ref[pair : pair + 2].reshape(2 * TGT_DEV, HEAD)
        s = lax.dot_general(q, k, (((1,), (1,)), ((), ())), preferred_element_type=f32)
        top = jnp.max(s, axis=1, keepdims=True)
        p = jnp.exp(s - top)
        total = jnp.sum(p, axis=1, keepdims=True)
        o = jnp.dot(p.astype(bf16), v, preferred_element_type=f32) / total
        o = o.astype(bf16)
        lse = top + jnp.log(total)
        for core in range(2):
            starts = [
                head * TGT_DEV + (2 * x + core) * BLOCK
                for head in (core, 1 - core)
                for x in range(4)
            ]
            for at, start in enumerate(starts):
                o_ref[pair + core, at * BLOCK : (at + 1) * BLOCK, :] = o[start : start + BLOCK]
            column = jnp.concatenate([lse[start : start + BLOCK] for start in starts], axis=0)
            line = jnp.broadcast_to(column, (TGT_DEV, TGT_DEV)).T[:1]
            hi = line.astype(bf16).astype(f32)
            mid = (line - hi).astype(bf16).astype(f32)
            lo = line - hi - mid
            first = jnp.concatenate([hi, mid], axis=1)
            second = jnp.concatenate([lo, jnp.zeros_like(lo)], axis=1)
            tile = jnp.where(row == 0, first, jnp.where(row == 1, second, 0.0))
            o_ref[pair + core, TGT_DEV:, :] = tile.astype(bf16)


def attend(queries, kv, step=4):
    blocks = queries.shape[0]
    return pl.pallas_call(
        attend_body,
        grid=(blocks // step,),
        in_specs=[
            pl.BlockSpec((step, TGT_DEV, HEAD), lambda i: (i, 0, 0)),
            pl.BlockSpec(kv.shape, lambda i: (0, 0)),
        ],
        out_specs=pl.BlockSpec((step, TGT_DEV + PAD, HEAD), lambda i: (i, 0, 0)),
        out_shape=jax.ShapeDtypeStruct((blocks, TGT_DEV + PAD, HEAD), bf16),
    )(queries, kv)


def merge_body(parts_ref, own_ref, other_ref, o_ref):
    count = parts_ref.shape[0]
    tail = parts_ref[:, TGT_DEV:, :].astype(f32)
    lse = tail[:, 0, :TGT_DEV] + tail[:, 0, TGT_DEV:] + tail[:, 1, :TGT_DEV]
    weight = jnp.exp(lse - jnp.max(lse, axis=0, keepdims=True))
    weight = (weight / jnp.sum(weight, axis=0, keepdims=True)).T
    merged = parts_ref[0, :TGT_DEV, :].astype(f32) * weight[:, :1]
    for t in range(1, count):
        merged = merged + parts_ref[t, :TGT_DEV, :].astype(f32) * weight[:, t : t + 1]
    merged = merged.astype(bf16)
    projected = jnp.dot(merged[:HALF], own_ref[...], preferred_element_type=f32)
    projected += jnp.dot(merged[HALF:], other_ref[...], preferred_element_type=f32)
    o_ref[...] = projected.astype(bf16)


def merge_project(parts, own, other):
    return pl.pallas_call(
        merge_body,
        out_shape=jax.ShapeDtypeStruct((HALF, D), bf16),
    )(parts, own, other)


def exchanged(array, axes):
    return lax.all_to_all(array, axes, 0, 0, tiled=True)


def sent_to_all(shard, axes):
    count = lax.axis_size(axes)
    return exchanged(jnp.broadcast_to(shard, (count, *shard.shape)), axes)


def summed_rows(partial):
    tiles = exchanged(partial.reshape(HALF // BLOCK, BLOCK, D), CHIPS)
    return jnp.sum(tiles.astype(f32), axis=0)


def other_core(array):
    return lax.ppermute(array, "c", [(0, 1), (1, 0)])


def from_last_line(array):
    lines = lax.axis_size(SP)
    axes = (*SP, "c")
    return lax.ppermute(array, axes, [(2 * i + 1, 2 * i + 2) for i in range(lines - 1)])


def shards(
    target,
    source,
    query_gain,
    source_gain,
    query_weight,
    key_weight,
    value_weight,
    out_weight,
    mixer_gain,
    gate_weight,
    up_weight,
    gate_taps,
    up_taps,
    down_weight,
    final_gain,
):
    first_mine = lax.axis_index(TP) * BLOCK
    source_normed = normalize(source, source_gain)
    key_rows = jnp.dot(source_normed, key_weight, preferred_element_type=f32).astype(bf16)
    value_rows = jnp.dot(source_normed, value_weight, preferred_element_type=f32).astype(bf16)
    rows = source.shape[0]
    by_head = jnp.stack(
        [
            jnp.concatenate([key_rows[:, :HEAD], value_rows[:, :HEAD]], axis=1),
            jnp.concatenate([key_rows[:, HEAD:], value_rows[:, HEAD:]], axis=1),
        ]
    )
    quads = lax.axis_size("q")
    to_send = jnp.broadcast_to(by_head[:, None], (KV_HEADS, quads, rows, 2 * HEAD))
    near = exchanged(to_send.reshape(KV_HEADS * quads, rows, 2 * HEAD), ("g", "q"))
    near = near.reshape(KV_HEADS * quads * rows, 2 * HEAD)
    near, target, out_weight, gate_weight, up_weight, gate_taps, up_taps, down_weight = (
        lax.optimization_barrier(
            (near, target, out_weight, gate_weight, up_weight, gate_taps, up_taps, down_weight)
        )
    )
    kv = lax.all_gather(near, "z", axis=0, tiled=True)

    normed = normalize(target, query_gain)
    own_query = jnp.dot(normed, query_weight, preferred_element_type=f32).astype(bf16)
    own_query = own_query * jnp.asarray(HEAD ** (-0.5), bf16)
    queries = sent_to_all(own_query, SLICES)
    out_other = other_core(out_weight)
    gate_other = other_core(gate_weight)
    up_other = other_core(up_weight)
    down_other = other_core(down_weight)
    taps = jnp.stack([gate_taps, up_taps])
    taps = jnp.concatenate([taps, other_core(taps)], axis=2).astype(f32)
    queries, out_other, gate_other, up_other, down_other, taps = lax.optimization_barrier(
        (queries, out_other, gate_other, up_other, down_other, taps)
    )

    parts = exchanged(attend(queries, kv), SLICES)
    projected = summed_rows(merge_project(parts, out_weight, out_other))
    target_rows = lax.dynamic_slice_in_dim(target, first_mine, BLOCK, 0)
    residual_rows = (target_rows.astype(f32) + projected).astype(bf16)
    arrived = sent_to_all(normalize(residual_rows, mixer_gain), CHIPS).reshape(HALF, D)
    gate_up = jnp.stack(
        [
            jnp.concatenate(
                [
                    jnp.dot(arrived, own, preferred_element_type=f32).astype(bf16),
                    jnp.dot(arrived, other, preferred_element_type=f32).astype(bf16),
                ],
                axis=1,
            )
            for own, other in ((gate_weight, gate_other), (up_weight, up_other))
        ]
    )
    width = gate_up.shape[2]
    blocks = gate_up.reshape(2, HALF // BLOCK, BLOCK, width)
    tails = blocks[:, :, BLOCK - (CONV - 1) :, :]
    across = other_core(tails)
    before = from_last_line(tails[:, -1:])
    shifted = jnp.concatenate([before, across[:, :-1]], axis=1)
    earlier = jnp.where(lax.axis_index("c") == 0, shifted, across)
    earlier = jnp.concatenate([earlier[..., width // 2 :], earlier[..., : width // 2]], axis=3)
    padded = jnp.concatenate([earlier, blocks], axis=2).astype(f32)
    mixed = taps[:, None, 0:1, :] * padded[:, :, 0:BLOCK, :]
    for tap in range(1, CONV):
        mixed = mixed + taps[:, None, tap : tap + 1, :] * padded[:, :, tap : tap + BLOCK, :]
    hidden = (jax.nn.silu(mixed[0]) * mixed[1]).astype(bf16).reshape(HALF, width)
    partial = jnp.dot(hidden[:, : width // 2], down_weight, preferred_element_type=f32)
    partial += jnp.dot(hidden[:, width // 2 :], down_other, preferred_element_type=f32)
    mixer = summed_rows(partial.astype(bf16))
    return normalize(residual_rows.astype(f32) + mixer, final_gain)


def solution(mesh):
    lines = mesh.shape["sp"]
    devices = mesh.devices.reshape(lines // 8, 8 // M, M, 2, 2, 2)
    split = Mesh(devices, SP + TP)
    whole = SP + TP
    return jax.shard_map(
        shards,
        mesh=split,
        in_specs=(
            P(SP, None),
            P(whole, None),
            P(),
            P(),
            P(None, TP),
            P(),
            P(),
            P(TP, None),
            P(),
            P(None, TP),
            P(None, TP),
            P(None, TP),
            P(None, TP),
            P(TP, None),
            P(),
        ),
        out_specs=P(whole, None),
        check_vma=False,
    )
```

```python
import jax
import jax.numpy as jnp
from jax import lax
from jax.experimental import pallas as pl
from jax.experimental.pallas import tpu as pltpu
from jax.sharding import Mesh
from jax.sharding import PartitionSpec as P

D = 2048
HEAD = 256
KV_HEADS = 2
CONV = 3
TGT_DEV = 128
PAD = 16
EPS = 1e-06

M = 4
SP = ("q", "m", "y")
TP = ("g", "xp", "c")
CHIPS = ("g", "xp")
SLICES = ("m", "xp")
BLOCK = 16
HALF = TGT_DEV // 2
bf16 = jnp.bfloat16
f32 = jnp.float32


def normalize(values, gain):
    widened = values.astype(f32)
    scaled = widened * lax.rsqrt(jnp.mean(widened * widened, axis=-1, keepdims=True) + EPS)
    return (scaled * gain).astype(bf16)


def attend_body(q_ref, own_ref, other_ref, o_ref):
    sources = (own_ref, other_ref)
    row = lax.broadcasted_iota(jnp.int32, (PAD, HEAD), 0)
    for at in range(0, q_ref.shape[0], 4):
        q = q_ref[at : at + 4].reshape(4 * HALF, HEAD)
        scores = [
            lax.dot_general(
                q, kv[:, :HEAD], (((1,), (1,)), ((), ())), preferred_element_type=f32
            )
            for kv in sources
        ]
        tops = [jnp.max(s, axis=1, keepdims=True) for s in scores]
        top = jnp.maximum(tops[0], tops[1])
        probs = [jnp.exp(s - top) for s in scores]
        total = sum(jnp.sum(p, axis=1, keepdims=True) for p in probs)
        o = sum(
            jnp.dot(p.astype(bf16), kv[:, HEAD:], preferred_element_type=f32)
            for p, kv in zip(probs, sources)
        )
        o = (o / total).astype(bf16)
        lse = top + jnp.log(total)
        for b in range(2):
            o_ref[at // 2 + b, :TGT_DEV, :] = o[b * TGT_DEV : (b + 1) * TGT_DEV]
            column = lse[b * TGT_DEV : (b + 1) * TGT_DEV]
            line = jnp.broadcast_to(column, (TGT_DEV, TGT_DEV)).T[:1]
            hi = line.astype(bf16).astype(f32)
            mid = (line - hi).astype(bf16).astype(f32)
            lo = line - hi - mid
            first = jnp.concatenate([hi, mid], axis=1)
            second = jnp.concatenate([lo, jnp.zeros_like(lo)], axis=1)
            tile = jnp.where(row == 0, first, jnp.where(row == 1, second, 0.0))
            o_ref[at // 2 + b, TGT_DEV:, :] = tile.astype(bf16)


def attend(queries, own, other, step=8):
    blocks = queries.shape[0]
    return pl.pallas_call(
        attend_body,
        grid=(blocks // step,),
        in_specs=[
            pl.BlockSpec((step, HALF, HEAD), lambda i: (i, 0, 0)),
            pl.BlockSpec(own.shape, lambda i: (0, 0)),
            pl.BlockSpec(other.shape, lambda i: (0, 0)),
        ],
        out_specs=pl.BlockSpec((step // 2, TGT_DEV + PAD, HEAD), lambda i: (i, 0, 0)),
        out_shape=jax.ShapeDtypeStruct((blocks // 2, TGT_DEV + PAD, HEAD), bf16),
    )(queries, own, other)


def merge_body(parts_ref, own_ref, other_ref, o_ref):
    count = parts_ref.shape[0]
    tail = parts_ref[:, TGT_DEV:, :].astype(f32)
    lse = tail[:, 0, :TGT_DEV] + tail[:, 0, TGT_DEV:] + tail[:, 1, :TGT_DEV]
    weight = jnp.exp(lse - jnp.max(lse, axis=0, keepdims=True))
    weight = (weight / jnp.sum(weight, axis=0, keepdims=True)).T
    merged = parts_ref[0, :TGT_DEV, :].astype(f32) * weight[:, :1]
    for t in range(1, count):
        merged = merged + parts_ref[t, :TGT_DEV, :].astype(f32) * weight[:, t : t + 1]
    merged = merged.astype(bf16)
    projected = jnp.dot(merged[:HALF], own_ref[...], preferred_element_type=f32)
    projected += jnp.dot(merged[HALF:], other_ref[...], preferred_element_type=f32)
    o_ref[...] = projected.astype(bf16)


def merge_project(parts, own, other):
    return pl.pallas_call(
        merge_body,
        out_shape=jax.ShapeDtypeStruct((HALF, D), bf16),
    )(parts, own, other)


def mixer_in_body(tiles_ref, target_ref, gain_ref, *refs):
    weights, (res_ref, gu_ref, tails_ref), held, sem = refs[:4], refs[4:7], refs[7], refs[8]
    copies = [pltpu.make_async_copy(w, held.at[k], sem.at[k]) for k, w in enumerate(weights)]
    for copy in copies:
        copy.start()
    projected = tiles_ref[0].astype(f32)
    for t in range(1, tiles_ref.shape[0]):
        projected = projected + tiles_ref[t].astype(f32)
    residual = (target_ref[...].astype(f32) + projected).astype(bf16)
    res_ref[...] = residual
    rows = normalize(residual, gain_ref[...])
    width = held.shape[2]
    for k, copy in enumerate(copies):
        copy.wait()
        part = jnp.dot(rows, held[k], preferred_element_type=f32).astype(bf16)
        gu_ref[:, k * width : (k + 1) * width] = part
        last = [part[b + BLOCK - (CONV - 1) : b + BLOCK] for b in range(0, HALF, BLOCK)]
        tails_ref[:, k * width : (k + 1) * width] = jnp.concatenate(last, axis=0)


def mixer_in(tiles, target, gain, weights):
    vmem = pl.BlockSpec(memory_space=pltpu.VMEM)
    hbm = pl.BlockSpec(memory_space=pl.ANY)
    width = weights[0].shape[1]
    count = len(weights)
    return pl.pallas_call(
        mixer_in_body,
        in_specs=[vmem, vmem, vmem] + [hbm] * count,
        out_shape=[
            jax.ShapeDtypeStruct((HALF, D), bf16),
            jax.ShapeDtypeStruct((HALF, count * width), bf16),
            jax.ShapeDtypeStruct((HALF // BLOCK * (CONV - 1), count * width), bf16),
        ],
        scratch_shapes=[
            pltpu.VMEM((count, D, width), bf16),
            pltpu.SemaphoreType.DMA((count,)),
        ],
    )(tiles, target, gain.reshape(1, D), *weights)


def mixer_out_body(core_ref, gu_ref, across_ref, before_ref, taps_ref, down_ref, other_ref, o_ref, held, sem):
    copies = [
        pltpu.make_async_copy(w, held.at[k], sem.at[k]) for k, w in enumerate((down_ref, other_ref))
    ]
    for copy in copies:
        copy.start()
    width = held.shape[1]
    halo = CONV - 1
    first = core_ref[0] == 0
    across = across_ref[...].astype(f32)
    before = before_ref[...].astype(f32)
    shifted = jnp.concatenate([before, across[:-halo]], axis=0)
    earlier = jnp.where(first, shifted, across)

    def convolved(at, from_at, tap_row, tap_at):
        blocks = []
        for b in range(HALF // BLOCK):
            ahead = earlier[b * halo : (b + 1) * halo, from_at : from_at + width]
            here = gu_ref[b * BLOCK : (b + 1) * BLOCK, at : at + width].astype(f32)
            padded = jnp.concatenate([ahead, here], axis=0)
            mixed = 0.0
            for tap in range(CONV):
                scale = taps_ref[tap_row + tap : tap_row + tap + 1, tap_at : tap_at + width]
                mixed = mixed + scale * padded[tap : tap + BLOCK]
            blocks.append(mixed)
        return jnp.concatenate(blocks, axis=0)

    total = 0.0
    for k, copy in enumerate(copies):
        gate = convolved(k * width, (1 - k) * width, 0, k * width)
        up = convolved((2 + k) * width, (3 - k) * width, CONV, k * width)
        hidden = (gate / (1.0 + jnp.exp(-gate)) * up).astype(bf16)
        copy.wait()
        total = total + jnp.dot(hidden, held[k], preferred_element_type=f32)
    o_ref[...] = total.astype(bf16)


def mixer_out(core, gate_up, across, before, taps, down, other):
    vmem = pl.BlockSpec(memory_space=pltpu.VMEM)
    hbm = pl.BlockSpec(memory_space=pl.ANY)
    return pl.pallas_call(
        mixer_out_body,
        in_specs=[pl.BlockSpec(memory_space=pltpu.SMEM), vmem, vmem, vmem, vmem, hbm, hbm],
        out_shape=jax.ShapeDtypeStruct((HALF, D), bf16),
        scratch_shapes=[pltpu.VMEM((2, *down.shape), bf16), pltpu.SemaphoreType.DMA((2,))],
    )(core, gate_up, across, before, taps, down, other)


def exchanged(array, axes):
    return lax.all_to_all(array, axes, 0, 0, tiled=True)


def sent_to_all(shard, axes):
    count = lax.axis_size(axes)
    return exchanged(jnp.broadcast_to(shard, (count, *shard.shape)), axes)


def other_core(array):
    return lax.ppermute(array, "c", [(0, 1), (1, 0)])


def from_last_line(array):
    lines = lax.axis_size(SP)
    axes = (*SP, "c")
    return lax.ppermute(array, axes, [(2 * i + 1, 2 * i + 2) for i in range(lines - 1)])


def shards(
    target,
    source,
    query_gain,
    source_gain,
    query_weight,
    key_weight,
    value_weight,
    out_weight,
    mixer_gain,
    gate_weight,
    up_weight,
    gate_taps,
    up_taps,
    down_weight,
    final_gain,
):
    core = lax.axis_index("c")
    chip = lax.axis_index(CHIPS)
    source_normed = normalize(source, source_gain)
    key_rows = jnp.dot(source_normed, key_weight, preferred_element_type=f32).astype(bf16)
    value_rows = jnp.dot(source_normed, value_weight, preferred_element_type=f32).astype(bf16)
    rows = source.shape[0]
    by_head = jnp.stack(
        [
            jnp.concatenate([key_rows[:, :HEAD], value_rows[:, :HEAD]], axis=1),
            jnp.concatenate([key_rows[:, HEAD:], value_rows[:, HEAD:]], axis=1),
        ]
    )
    quads = lax.axis_size("q")
    to_send = jnp.broadcast_to(by_head[:, None], (KV_HEADS, quads, rows, 2 * HEAD))
    near = exchanged(to_send.reshape(KV_HEADS * quads, rows, 2 * HEAD), ("g", "q"))
    near = near.reshape(KV_HEADS * quads * rows, 2 * HEAD)
    near, target, out_weight, gate_weight, up_weight, gate_taps, up_taps, down_weight = (
        lax.optimization_barrier(
            (near, target, out_weight, gate_weight, up_weight, gate_taps, up_taps, down_weight)
        )
    )
    kv = sent_to_all(near, "y").reshape(-1, 2 * HEAD)

    normed = normalize(target, query_gain)
    own_query = jnp.dot(normed, query_weight, preferred_element_type=f32).astype(bf16)
    own_query = own_query * jnp.asarray(HEAD ** (-0.5), bf16)
    by_core = own_query.reshape(4, 2, BLOCK, HEAD)
    kept = lax.dynamic_index_in_dim(by_core, core, 1, False).reshape(HALF, HEAD)
    given = lax.dynamic_index_in_dim(by_core, 1 - core, 1, False).reshape(HALF, HEAD)
    both = jnp.stack([kept, other_core(given)])
    queries = lax.all_gather(both, "xp", axis=0, tiled=True)
    queries = lax.all_gather(queries, "m", axis=0, tiled=True)
    target_half = lax.dynamic_index_in_dim(target.reshape(4, 2, BLOCK, D), core, 1, False)
    target_half = target_half.reshape(HALF, D)
    out_other = other_core(out_weight)
    gate_other = other_core(gate_weight)
    up_other = other_core(up_weight)
    down_other = other_core(down_weight)
    taps = jnp.concatenate([gate_taps, up_taps], axis=0)
    taps = jnp.concatenate([taps, other_core(taps)], axis=1).astype(f32)
    queries, target_half, out_other, gate_other, up_other, down_other, taps = (
        lax.optimization_barrier(
            (queries, target_half, out_other, gate_other, up_other, down_other, taps)
        )
    )
    parts = exchanged(attend(queries, kv, other_core(kv)), SLICES)
    core_at = core.astype(jnp.int32).reshape(1)
    partial = merge_project(parts, out_weight, out_other)
    residual, gate_up, tails = mixer_in(
        sent_to_all(partial, CHIPS),
        target_half,
        mixer_gain,
        (gate_weight, gate_other, up_weight, up_other),
    )
    before = from_last_line(tails[-(CONV - 1) :])
    across = other_core(tails)
    partial = mixer_out(core_at, gate_up, across, before, taps, down_weight, down_other)
    tiles = exchanged(partial.reshape(HALF // BLOCK, BLOCK, D), CHIPS)
    mixer = jnp.sum(tiles.astype(f32), axis=0)
    own_rows = lax.dynamic_slice_in_dim(residual, chip * BLOCK, BLOCK, 0)
    return normalize(own_rows.astype(f32) + mixer, final_gain)


def solution(mesh):
    lines = mesh.shape["sp"]
    devices = mesh.devices.reshape(lines // 8 // M, M, 8, 2, 2, 2)
    split = Mesh(devices, SP + TP)
    whole = SP + TP
    return jax.shard_map(
        shards,
        mesh=split,
        in_specs=(
            P(SP, None),
            P(whole, None),
            P(),
            P(),
            P(None, TP),
            P(),
            P(),
            P(TP, None),
            P(),
            P(None, TP),
            P(None, TP),
            P(None, TP),
            P(None, TP),
            P(TP, None),
            P(),
        ),
        out_specs=P(whole, None),
        check_vma=False,
    )
```

```python
import jax
import jax.numpy as jnp
from jax import lax
from jax.experimental import pallas as pl
from jax.experimental.pallas import tpu as pltpu
from jax.sharding import Mesh
from jax.sharding import PartitionSpec as P

D = 2048
HEAD = 256
KV_HEADS = 2
CONV = 3
TGT_DEV = 128
PAD = 16
EPS = 1e-06

SP = ("zq", "zm", "ym", "yq")
TP = ("g", "xp", "c")
CHIPS = ("g", "xp")
SLICES = ("ym", "zm")
SAME_SLICE = ("yq", "zq")
BLOCK = 16
HALF = TGT_DEV // 2
bf16 = jnp.bfloat16
f32 = jnp.float32


def normalize(values, gain):
    widened = values.astype(f32)
    scaled = widened * lax.rsqrt(jnp.mean(widened * widened, axis=-1, keepdims=True) + EPS)
    return (scaled * gain).astype(bf16)


def attend_body(q_ref, own_ref, other_ref, o_ref):
    sources = (own_ref, other_ref)
    row = lax.broadcasted_iota(jnp.int32, (PAD, HEAD), 0)
    for at in range(0, q_ref.shape[0], 4):
        q = q_ref[at : at + 4].reshape(4 * HALF, HEAD)
        scores = [
            lax.dot_general(
                q, kv[:, :HEAD], (((1,), (1,)), ((), ())), preferred_element_type=f32
            )
            for kv in sources
        ]
        tops = [jnp.max(s, axis=1, keepdims=True) for s in scores]
        top = jnp.maximum(tops[0], tops[1])
        probs = [jnp.exp(s - top) for s in scores]
        total = sum(jnp.sum(p, axis=1, keepdims=True) for p in probs)
        o = sum(
            jnp.dot(p.astype(bf16), kv[:, HEAD:], preferred_element_type=f32)
            for p, kv in zip(probs, sources)
        )
        o = (o / total).astype(bf16)
        lse = top + jnp.log(total)
        for b in range(2):
            o_ref[at // 2 + b, :TGT_DEV, :] = o[b * TGT_DEV : (b + 1) * TGT_DEV]
            column = lse[b * TGT_DEV : (b + 1) * TGT_DEV]
            line = jnp.broadcast_to(column, (TGT_DEV, TGT_DEV)).T[:1]
            hi = line.astype(bf16).astype(f32)
            mid = (line - hi).astype(bf16).astype(f32)
            lo = line - hi - mid
            first = jnp.concatenate([hi, mid], axis=1)
            second = jnp.concatenate([lo, jnp.zeros_like(lo)], axis=1)
            tile = jnp.where(row == 0, first, jnp.where(row == 1, second, 0.0))
            o_ref[at // 2 + b, TGT_DEV:, :] = tile.astype(bf16)


def attend(queries, own, other, step=8):
    blocks = queries.shape[0]
    return pl.pallas_call(
        attend_body,
        grid=(blocks // step,),
        in_specs=[
            pl.BlockSpec((step, HALF, HEAD), lambda i: (i, 0, 0)),
            pl.BlockSpec(own.shape, lambda i: (0, 0)),
            pl.BlockSpec(other.shape, lambda i: (0, 0)),
        ],
        out_specs=pl.BlockSpec((step // 2, TGT_DEV + PAD, HEAD), lambda i: (i, 0, 0)),
        out_shape=jax.ShapeDtypeStruct((blocks // 2, TGT_DEV + PAD, HEAD), bf16),
    )(queries, own, other)


def merge_body(parts_hbm, own_hbm, other_hbm, o_ref, parts_ref, held, sem):
    arrive = pltpu.make_async_copy(parts_hbm, parts_ref, sem.at[2])
    arrive.start()
    copies = [
        pltpu.make_async_copy(w, held.at[k], sem.at[k]) for k, w in enumerate((own_hbm, other_hbm))
    ]
    for copy in copies:
        copy.start()
    arrive.wait()
    count = parts_ref.shape[0]
    tail = parts_ref[:, TGT_DEV:, :].astype(f32)
    lse = tail[:, 0, :TGT_DEV] + tail[:, 0, TGT_DEV:] + tail[:, 1, :TGT_DEV]
    weight = jnp.exp(lse - jnp.max(lse, axis=0, keepdims=True))
    weight = (weight / jnp.sum(weight, axis=0, keepdims=True)).T
    merged = parts_ref[0, :TGT_DEV, :].astype(f32) * weight[:, :1]
    for t in range(1, count):
        merged = merged + parts_ref[t, :TGT_DEV, :].astype(f32) * weight[:, t : t + 1]
    merged = merged.astype(bf16)
    copies[0].wait()
    projected = jnp.dot(merged[:HALF], held[0], preferred_element_type=f32)
    copies[1].wait()
    projected += jnp.dot(merged[HALF:], held[1], preferred_element_type=f32)
    projected = projected.astype(bf16)
    for t in range(o_ref.shape[0]):
        o_ref[t] = projected


def merge_project(parts, own, other, copies):
    hbm = pl.BlockSpec(memory_space=pl.ANY)
    return pl.pallas_call(
        merge_body,
        in_specs=[hbm] * 3,
        out_shape=jax.ShapeDtypeStruct((copies, HALF, D), bf16),
        scratch_shapes=[
            pltpu.VMEM(parts.shape, bf16),
            pltpu.VMEM((2, *own.shape), bf16),
            pltpu.SemaphoreType.DMA((3,)),
        ],
    )(parts, own, other)


def mixer_in_body(tiles_hbm, target_hbm, gain_ref, *refs):
    weights, (res_ref, gu_ref, tails_ref, last_ref) = refs[:4], refs[4:8]
    tiles_ref, target_ref, held, sem = refs[8:]
    arrive = [
        pltpu.make_async_copy(tiles_hbm, tiles_ref, sem.at[4]),
        pltpu.make_async_copy(target_hbm, target_ref, sem.at[5]),
    ]
    copies = [pltpu.make_async_copy(w, held.at[k], sem.at[k]) for k, w in enumerate(weights)]
    for copy in arrive + copies:
        copy.start()
    for copy in arrive:
        copy.wait()
    projected = tiles_ref[0].astype(f32)
    for t in range(1, tiles_ref.shape[0]):
        projected = projected + tiles_ref[t].astype(f32)
    residual = (target_ref[...].astype(f32) + projected).astype(bf16)
    res_ref[...] = residual
    rows = normalize(residual, gain_ref[...])
    width = held.shape[2]
    for k, copy in enumerate(copies):
        copy.wait()
        part = jnp.dot(rows, held[k], preferred_element_type=f32).astype(bf16)
        gu_ref[:, k * width : (k + 1) * width] = part
        last = [part[b + BLOCK - (CONV - 1) : b + BLOCK] for b in range(0, HALF, BLOCK)]
        tails_ref[:, k * width : (k + 1) * width] = jnp.concatenate(last, axis=0)
        last_ref[:, k * width : (k + 1) * width] = last[-1]


def mixer_in(tiles, target, gain, weights):
    vmem = pl.BlockSpec(memory_space=pltpu.VMEM)
    hbm = pl.BlockSpec(memory_space=pl.ANY)
    width = weights[0].shape[1]
    count = len(weights)
    return pl.pallas_call(
        mixer_in_body,
        in_specs=[hbm, hbm, vmem] + [hbm] * count,
        out_shape=[
            jax.ShapeDtypeStruct((HALF, D), bf16),
            jax.ShapeDtypeStruct((HALF, count * width), bf16),
            jax.ShapeDtypeStruct((HALF // BLOCK * (CONV - 1), count * width), bf16),
            jax.ShapeDtypeStruct((CONV - 1, count * width), bf16),
        ],
        scratch_shapes=[
            pltpu.VMEM(tiles.shape, bf16),
            pltpu.VMEM(target.shape, bf16),
            pltpu.VMEM((count, D, width), bf16),
            pltpu.SemaphoreType.DMA((count + 2,)),
        ],
    )(tiles, target, gain.reshape(1, D), *weights)


def mixer_out_body(core_ref, gu_ref, across_ref, before_ref, taps_ref, down_ref, other_ref, o_ref, held, sem):
    copies = [
        pltpu.make_async_copy(w, held.at[k], sem.at[k]) for k, w in enumerate((down_ref, other_ref))
    ]
    for copy in copies:
        copy.start()
    width = held.shape[1]
    halo = CONV - 1
    first = core_ref[0] == 0
    across = across_ref[...].astype(f32)
    before = before_ref[...].astype(f32)
    shifted = jnp.concatenate([before, across[:-halo]], axis=0)
    earlier = jnp.where(first, shifted, across)

    place = lax.broadcasted_iota(jnp.int32, (HALF, width), 0) % BLOCK

    def spread(row, from_at):
        return jnp.concatenate(
            [
                jnp.broadcast_to(
                    earlier[b * halo + row : b * halo + row + 1, from_at : from_at + width],
                    (BLOCK, width),
                )
                for b in range(HALF // BLOCK)
            ],
            axis=0,
        )

    def convolved(at, from_at, tap_row, tap_at):
        here = gu_ref[:, at : at + width].astype(f32)
        last = spread(1, from_at)
        one = jnp.where(place == 0, last, pltpu.roll(here, 1, 0))
        two = jnp.where(place == 1, last, pltpu.roll(here, 2, 0))
        two = jnp.where(place == 0, spread(0, from_at), two)
        scale = taps_ref[tap_row : tap_row + CONV, tap_at : tap_at + width]
        return scale[0:1] * two + scale[1:2] * one + scale[2:3] * here

    total = 0.0
    for k, copy in enumerate(copies):
        gate = convolved(k * width, (1 - k) * width, 0, k * width)
        up = convolved((2 + k) * width, (3 - k) * width, CONV, k * width)
        hidden = (gate / (1.0 + jnp.exp(-gate)) * up).astype(bf16)
        copy.wait()
        total = total + jnp.dot(hidden, held[k], preferred_element_type=f32)
    o_ref[...] = total.astype(bf16)


def mixer_out(core, gate_up, across, before, taps, down, other):
    vmem = pl.BlockSpec(memory_space=pltpu.VMEM)
    hbm = pl.BlockSpec(memory_space=pl.ANY)
    return pl.pallas_call(
        mixer_out_body,
        in_specs=[pl.BlockSpec(memory_space=pltpu.SMEM), vmem, vmem, vmem, vmem, hbm, hbm],
        out_shape=jax.ShapeDtypeStruct((HALF, D), bf16),
        scratch_shapes=[pltpu.VMEM((2, *down.shape), bf16), pltpu.SemaphoreType.DMA((2,))],
    )(core, gate_up, across, before, taps, down, other)


def exchanged(array, axes):
    return lax.all_to_all(array, axes, 0, 0, tiled=True)


def sent_to_all(shard, axes):
    count = lax.axis_size(axes)
    return exchanged(jnp.broadcast_to(shard, (count, *shard.shape)), axes)


def other_core(array):
    return lax.ppermute(array, "c", [(0, 1), (1, 0)])


def from_last_line(array):
    lines = lax.axis_size(SP)
    axes = (*SP, "c")
    return lax.ppermute(array, axes, [(2 * i + 1, 2 * i + 2) for i in range(lines - 1)])


def shards(
    target,
    source,
    query_gain,
    source_gain,
    query_weight,
    key_weight,
    value_weight,
    out_weight,
    mixer_gain,
    gate_weight,
    up_weight,
    gate_taps,
    up_taps,
    down_weight,
    final_gain,
):
    core = lax.axis_index("c")
    chip = lax.axis_index(CHIPS)
    source_normed = normalize(source, source_gain)
    key_rows = jnp.dot(source_normed, key_weight, preferred_element_type=f32).astype(bf16)
    value_rows = jnp.dot(source_normed, value_weight, preferred_element_type=f32).astype(bf16)
    rows = source.shape[0]
    by_head = jnp.stack(
        [
            jnp.concatenate([key_rows[:, :HEAD], value_rows[:, :HEAD]], axis=1),
            jnp.concatenate([key_rows[:, HEAD:], value_rows[:, HEAD:]], axis=1),
        ]
    )
    near_lines = lax.axis_size(SAME_SLICE)
    by_head = by_head.reshape(KV_HEADS * rows, 2 * HEAD)
    near = sent_to_all(by_head, SAME_SLICE)
    near = near.reshape(near_lines, KV_HEADS, rows, 2 * HEAD).transpose(1, 0, 2, 3)
    near = near.reshape(KV_HEADS, 1, near_lines * rows, 2 * HEAD)
    chips = lax.axis_size(CHIPS)
    near = jnp.broadcast_to(near, (KV_HEADS, chips // KV_HEADS, *near.shape[2:]))
    kv = exchanged(near.reshape(chips, *near.shape[2:]), CHIPS).reshape(-1, 2 * HEAD)

    normed = normalize(target, query_gain)
    own_query = jnp.dot(normed, query_weight, preferred_element_type=f32).astype(bf16)
    own_query = own_query * jnp.asarray(HEAD ** (-0.5), bf16)
    by_core = own_query.reshape(4, 2, BLOCK, HEAD)
    kept = lax.dynamic_index_in_dim(by_core, core, 1, False).reshape(HALF, HEAD)
    given = lax.dynamic_index_in_dim(by_core, 1 - core, 1, False).reshape(HALF, HEAD)
    given = other_core(given)
    both = jnp.stack([kept, given])
    queries = lax.all_gather(both[None], "zm", axis=0, tiled=True)
    queries = lax.all_gather(queries[None], "ym", axis=0, tiled=True)
    queries = queries.reshape(-1, HALF, HEAD)
    target_half = lax.dynamic_index_in_dim(target.reshape(4, 2, BLOCK, D), core, 1, False)
    target_half = target_half.reshape(HALF, D)
    taps = jnp.concatenate([gate_taps, up_taps], axis=0)
    out_other = other_core(out_weight)
    gate_other = other_core(gate_weight)
    up_other = other_core(up_weight)
    down_other = other_core(down_weight)
    taps_other = other_core(taps)
    taps = jnp.concatenate([taps, taps_other], axis=1).astype(f32)
    queries, target_half, out_other, gate_other, up_other, down_other, taps = (
        lax.optimization_barrier(
            (queries, target_half, out_other, gate_other, up_other, down_other, taps)
        )
    )
    parts = exchanged(attend(queries, kv, other_core(kv)), SLICES)
    core_at = core.astype(jnp.int32).reshape(1)
    partial = merge_project(parts, out_weight, out_other, chips)
    residual, gate_up, tails, last = mixer_in(
        exchanged(partial, CHIPS),
        target_half,
        mixer_gain,
        (gate_weight, gate_other, up_weight, up_other),
    )
    before = from_last_line(last)
    across = other_core(tails)
    partial = mixer_out(core_at, gate_up, across, before, taps, down_weight, down_other)
    tiles = exchanged(partial.reshape(HALF // BLOCK, BLOCK, D), CHIPS)
    mixer = jnp.sum(tiles.astype(f32), axis=0)
    own_rows = lax.dynamic_slice_in_dim(residual, chip * BLOCK, BLOCK, 0)
    return normalize(own_rows.astype(f32) + mixer, final_gain)


def solution(mesh):
    lines = mesh.shape["sp"]
    devices = mesh.devices.reshape(lines // 32, 4, 2, 4, 2, 2, 2)
    split = Mesh(devices, SP + TP)
    whole = SP + TP
    return jax.shard_map(
        shards,
        mesh=split,
        in_specs=(
            P(SP, None),
            P(whole, None),
            P(),
            P(),
            P(None, TP),
            P(),
            P(),
            P(TP, None),
            P(),
            P(None, TP),
            P(None, TP),
            P(None, TP),
            P(None, TP),
            P(TP, None),
            P(),
        ),
        out_specs=P(whole, None),
        check_vma=False,
    )
```

```python
import jax
import jax.numpy as jnp
from jax import lax
from jax.experimental import pallas as pl
from jax.experimental.pallas import tpu as pltpu
from jax.sharding import Mesh
from jax.sharding import PartitionSpec as P

D = 2048
HEAD = 256
KV_HEADS = 2
CONV = 3
TGT_DEV = 128
PAD = 16
EPS = 1e-06

SP = ("zq", "zm", "ym", "yq")
TP = ("g", "xp", "c")
CHIPS = ("g", "xp")
SLICES = ("zm", "ym")
SAME_SLICE = ("yq", "zq")
BLOCK = 16
HALF = TGT_DEV // 2
bf16 = jnp.bfloat16
f32 = jnp.float32


def normalize(values, gain):
    widened = values.astype(f32)
    scaled = widened * lax.rsqrt(jnp.mean(widened * widened, axis=-1, keepdims=True) + EPS)
    return (scaled * gain).astype(bf16)


def attend_body(line_ref, q_ref, own_ref, other_ref, o_ref):
    sources = (own_ref, other_ref)
    row = lax.broadcasted_iota(jnp.int32, (PAD, HEAD), 0)
    lines = q_ref.shape[0] // 2
    base = pl.program_id(0) * o_ref.shape[0]
    for at in range(0, o_ref.shape[0] * 2, 4):
        pieces = [
            q_ref[pl.ds(2 * ((line_ref[0] + lines - (base + at // 2 + b)) % lines), 2)]
            for b in range(2)
        ]
        q = jnp.concatenate(pieces, axis=0).reshape(4 * HALF, HEAD)
        scores = [
            lax.dot_general(
                q, kv[:, :HEAD], (((1,), (1,)), ((), ())), preferred_element_type=f32
            )
            for kv in sources
        ]
        tops = [jnp.max(s, axis=1, keepdims=True) for s in scores]
        top = jnp.maximum(tops[0], tops[1])
        probs = [jnp.exp(s - top) for s in scores]
        total = sum(jnp.sum(p, axis=1, keepdims=True) for p in probs)
        o = sum(
            jnp.dot(p.astype(bf16), kv[:, HEAD:], preferred_element_type=f32)
            for p, kv in zip(probs, sources)
        )
        o = (o / total).astype(bf16)
        lse = top + jnp.log(total)
        for b in range(2):
            o_ref[at // 2 + b, :TGT_DEV, :] = o[b * TGT_DEV : (b + 1) * TGT_DEV]
            column = lse[b * TGT_DEV : (b + 1) * TGT_DEV]
            line = jnp.broadcast_to(column, (TGT_DEV, TGT_DEV)).T[:1]
            hi = line.astype(bf16).astype(f32)
            mid = (line - hi).astype(bf16).astype(f32)
            lo = line - hi - mid
            first = jnp.concatenate([hi, mid], axis=1)
            second = jnp.concatenate([lo, jnp.zeros_like(lo)], axis=1)
            tile = jnp.where(row == 0, first, jnp.where(row == 1, second, 0.0))
            o_ref[at // 2 + b, TGT_DEV:, :] = tile.astype(bf16)


def attend(line, queries, own, other, step=4):
    blocks = queries.shape[0] // 2
    whole = pl.BlockSpec(queries.shape, lambda i: (0, 0, 0))
    return pl.pallas_call(
        attend_body,
        grid=(blocks // step,),
        in_specs=[
            pl.BlockSpec(memory_space=pltpu.SMEM),
            whole,
            pl.BlockSpec(own.shape, lambda i: (0, 0)),
            pl.BlockSpec(other.shape, lambda i: (0, 0)),
        ],
        out_specs=pl.BlockSpec((step, TGT_DEV + PAD, HEAD), lambda i: (i, 0, 0)),
        out_shape=pltpu.VMEM((blocks, TGT_DEV + PAD, HEAD), bf16),
    )(line, queries, own, other)


def merge_body(parts_ref, own_hbm, other_hbm, o_ref, held, sem):
    copies = [
        pltpu.make_async_copy(w, held.at[k], sem.at[k]) for k, w in enumerate((own_hbm, other_hbm))
    ]
    for copy in copies:
        copy.start()
    count = parts_ref.shape[0]
    tail = parts_ref[:, TGT_DEV:, :].astype(f32)
    lse = tail[:, 0, :TGT_DEV] + tail[:, 0, TGT_DEV:] + tail[:, 1, :TGT_DEV]
    weight = jnp.exp(lse - jnp.max(lse, axis=0, keepdims=True))
    weight = (weight / jnp.sum(weight, axis=0, keepdims=True)).T
    merged = parts_ref[0, :TGT_DEV, :].astype(f32) * weight[:, :1]
    for t in range(1, count):
        merged = merged + parts_ref[t, :TGT_DEV, :].astype(f32) * weight[:, t : t + 1]
    merged = merged.astype(bf16)
    copies[0].wait()
    projected = jnp.dot(merged[:HALF], held[0], preferred_element_type=f32)
    copies[1].wait()
    projected += jnp.dot(merged[HALF:], held[1], preferred_element_type=f32)
    projected = projected.astype(bf16)
    for t in range(o_ref.shape[0]):
        o_ref[t] = projected


def in_vmem(array):
    return pltpu.with_memory_space_constraint(array, pltpu.VMEM)


def merge_project(parts, own, other, copies):
    hbm = pl.BlockSpec(memory_space=pl.ANY)
    return pl.pallas_call(
        merge_body,
        in_specs=[pl.BlockSpec(memory_space=pltpu.VMEM), hbm, hbm],
        out_shape=jax.ShapeDtypeStruct((copies, HALF, D), bf16),
        scratch_shapes=[pltpu.VMEM((2, *own.shape), bf16), pltpu.SemaphoreType.DMA((2,))],
    )(in_vmem(parts), own, other)


def mixer_in_body(tiles_ref, target_hbm, gain_ref, *refs):
    weights, (res_ref, gu_ref, tails_ref, last_ref) = refs[:4], refs[4:8]
    target_ref, held, sem = refs[8:]
    arrive = pltpu.make_async_copy(target_hbm, target_ref, sem.at[4])
    arrive.start()
    copies = [pltpu.make_async_copy(w, held.at[k], sem.at[k]) for k, w in enumerate(weights)]
    for copy in copies:
        copy.start()
    arrive.wait()
    projected = tiles_ref[0].astype(f32)
    for t in range(1, tiles_ref.shape[0]):
        projected = projected + tiles_ref[t].astype(f32)
    residual = (target_ref[...].astype(f32) + projected).astype(bf16)
    res_ref[...] = residual
    rows = normalize(residual, gain_ref[...])
    width = held.shape[2]
    for k, copy in enumerate(copies):
        copy.wait()
        part = jnp.dot(rows, held[k], preferred_element_type=f32).astype(bf16)
        gu_ref[:, k * width : (k + 1) * width] = part
        last = [part[b + BLOCK - (CONV - 1) : b + BLOCK] for b in range(0, HALF, BLOCK)]
        tails_ref[:, k * width : (k + 1) * width] = jnp.concatenate(last, axis=0)
        last_ref[:, k * width : (k + 1) * width] = last[-1]


def mixer_in(tiles, target, gain, weights):
    vmem = pl.BlockSpec(memory_space=pltpu.VMEM)
    hbm = pl.BlockSpec(memory_space=pl.ANY)
    width = weights[0].shape[1]
    count = len(weights)
    return pl.pallas_call(
        mixer_in_body,
        in_specs=[vmem, hbm, vmem] + [hbm] * count,
        out_shape=[
            pltpu.VMEM((HALF, D), bf16),
            pltpu.VMEM((HALF, count * width), bf16),
            pltpu.VMEM((HALF // BLOCK * (CONV - 1), count * width), bf16),
            pltpu.VMEM((CONV - 1, count * width), bf16),
        ],
        scratch_shapes=[
            pltpu.VMEM(target.shape, bf16),
            pltpu.VMEM((count, D, width), bf16),
            pltpu.SemaphoreType.DMA((count + 1,)),
        ],
    )(in_vmem(tiles), target, gain.reshape(1, D), *weights)


def mixer_out_body(core_ref, gu_ref, across_ref, before_ref, taps_ref, down_ref, other_ref, o_ref, held, sem):
    copies = [
        pltpu.make_async_copy(w, held.at[k], sem.at[k]) for k, w in enumerate((down_ref, other_ref))
    ]
    for copy in copies:
        copy.start()
    width = held.shape[1]
    halo = CONV - 1
    first = core_ref[0] == 0
    across = across_ref[...].astype(f32)
    before = before_ref[...].astype(f32)
    shifted = jnp.concatenate([before, across[:-halo]], axis=0)
    earlier = jnp.where(first, shifted, across)

    place = lax.broadcasted_iota(jnp.int32, (HALF, width), 0) % BLOCK

    def spread(row, from_at):
        return jnp.concatenate(
            [
                jnp.broadcast_to(
                    earlier[b * halo + row : b * halo + row + 1, from_at : from_at + width],
                    (BLOCK, width),
                )
                for b in range(HALF // BLOCK)
            ],
            axis=0,
        )

    def convolved(at, from_at, tap_row, tap_at):
        here = gu_ref[:, at : at + width].astype(f32)
        last = spread(1, from_at)
        one = jnp.where(place == 0, last, pltpu.roll(here, 1, 0))
        two = jnp.where(place == 1, last, pltpu.roll(here, 2, 0))
        two = jnp.where(place == 0, spread(0, from_at), two)
        scale = taps_ref[tap_row : tap_row + CONV, tap_at : tap_at + width]
        return scale[0:1] * two + scale[1:2] * one + scale[2:3] * here

    total = 0.0
    for k, copy in enumerate(copies):
        gate = convolved(k * width, (1 - k) * width, 0, k * width)
        up = convolved((2 + k) * width, (3 - k) * width, CONV, k * width)
        hidden = (gate / (1.0 + jnp.exp(-gate)) * up).astype(bf16)
        copy.wait()
        total = total + jnp.dot(hidden, held[k], preferred_element_type=f32)
    o_ref[...] = total.astype(bf16)


def mixer_out(core, gate_up, across, before, taps, down, other):
    vmem = pl.BlockSpec(memory_space=pltpu.VMEM)
    hbm = pl.BlockSpec(memory_space=pl.ANY)
    return pl.pallas_call(
        mixer_out_body,
        in_specs=[pl.BlockSpec(memory_space=pltpu.SMEM), vmem, vmem, vmem, vmem, hbm, hbm],
        out_shape=pltpu.VMEM((HALF, D), bf16),
        scratch_shapes=[pltpu.VMEM((2, *down.shape), bf16), pltpu.SemaphoreType.DMA((2,))],
    )(core, in_vmem(gate_up), in_vmem(across), in_vmem(before), taps, down, other)


def exchanged(array, axes):
    return lax.all_to_all(array, axes, 0, 0, tiled=True)


def sent_to_all(shard, axes):
    count = lax.axis_size(axes)
    return exchanged(jnp.broadcast_to(shard, (count, *shard.shape)), axes)


def other_core(array):
    return lax.ppermute(array, "c", [(0, 1), (1, 0)])


def from_last_line(array):
    lines = lax.axis_size(SP)
    axes = (*SP, "c")
    return lax.ppermute(array, axes, [(2 * i + 1, 2 * i + 2) for i in range(lines - 1)])


def shards(
    target,
    source,
    query_gain,
    source_gain,
    query_weight,
    key_weight,
    value_weight,
    out_weight,
    mixer_gain,
    gate_weight,
    up_weight,
    gate_taps,
    up_taps,
    down_weight,
    final_gain,
):
    core = lax.axis_index("c")
    chip = lax.axis_index(CHIPS)
    source_normed = normalize(source, source_gain)
    key_rows = jnp.dot(source_normed, key_weight, preferred_element_type=f32).astype(bf16)
    value_rows = jnp.dot(source_normed, value_weight, preferred_element_type=f32).astype(bf16)
    rows = source.shape[0]
    by_head = jnp.stack(
        [
            jnp.concatenate([key_rows[:, :HEAD], value_rows[:, :HEAD]], axis=1),
            jnp.concatenate([key_rows[:, HEAD:], value_rows[:, HEAD:]], axis=1),
        ]
    )
    near_lines = lax.axis_size(SAME_SLICE)
    by_head = by_head.reshape(KV_HEADS * rows, 2 * HEAD)
    near = sent_to_all(by_head, SAME_SLICE)
    near = near.reshape(near_lines, KV_HEADS, rows, 2 * HEAD).transpose(1, 0, 2, 3)
    near = near.reshape(KV_HEADS, 1, near_lines * rows, 2 * HEAD)
    chips = lax.axis_size(CHIPS)
    near = jnp.broadcast_to(near, (KV_HEADS, chips // KV_HEADS, *near.shape[2:]))
    kv = exchanged(near.reshape(chips, *near.shape[2:]), CHIPS).reshape(-1, 2 * HEAD)

    normed = normalize(target, query_gain)
    own_query = jnp.dot(normed, query_weight, preferred_element_type=f32).astype(bf16)
    own_query = own_query * jnp.asarray(HEAD ** (-0.5), bf16)
    by_core = own_query.reshape(4, 2, BLOCK, HEAD)
    kept = lax.dynamic_index_in_dim(by_core, core, 1, False).reshape(HALF, HEAD)
    given = lax.dynamic_index_in_dim(by_core, 1 - core, 1, False).reshape(HALF, HEAD)
    given = other_core(given)
    both = jnp.stack([kept, given])
    lines = lax.axis_size(SLICES)
    queries = [both]
    for by in range(1, lines):
        pairs = [(i, (i + by) % lines) for i in range(lines)]
        queries.append(lax.ppermute(both, SLICES, pairs))
    queries = jnp.concatenate(queries, axis=0)
    target_half = lax.dynamic_index_in_dim(target.reshape(4, 2, BLOCK, D), core, 1, False)
    target_half = target_half.reshape(HALF, D)
    taps = jnp.concatenate([gate_taps, up_taps], axis=0)
    out_other = other_core(out_weight)
    gate_other = other_core(gate_weight)
    up_other = other_core(up_weight)
    down_other = other_core(down_weight)
    taps_other = other_core(taps)
    taps = jnp.concatenate([taps, taps_other], axis=1).astype(f32)
    queries, target_half, out_other, gate_other, up_other, down_other, taps = (
        lax.optimization_barrier(
            (queries, target_half, out_other, gate_other, up_other, down_other, taps)
        )
    )
    line_at = lax.axis_index(SLICES).astype(jnp.int32).reshape(1)
    parts = exchanged(attend(line_at, queries, kv, other_core(kv)), SLICES)
    core_at = core.astype(jnp.int32).reshape(1)
    partial = merge_project(parts, out_weight, out_other, chips)
    residual, gate_up, tails, last = mixer_in(
        exchanged(partial, CHIPS),
        target_half,
        mixer_gain,
        (gate_weight, gate_other, up_weight, up_other),
    )
    before = from_last_line(last)
    across = other_core(tails)
    partial = mixer_out(core_at, gate_up, across, before, taps, down_weight, down_other)
    tiles = exchanged(partial.reshape(HALF // BLOCK, BLOCK, D), CHIPS)
    mixer = jnp.sum(tiles.astype(f32), axis=0)
    own_rows = lax.dynamic_slice_in_dim(residual, chip * BLOCK, BLOCK, 0)
    return normalize(own_rows.astype(f32) + mixer, final_gain)


def solution(mesh):
    lines = mesh.shape["sp"]
    devices = mesh.devices.reshape(lines // 32, 4, 2, 4, 2, 2, 2)
    split = Mesh(devices, SP + TP)
    whole = SP + TP
    return jax.shard_map(
        shards,
        mesh=split,
        in_specs=(
            P(SP, None),
            P(whole, None),
            P(),
            P(),
            P(None, TP),
            P(),
            P(),
            P(TP, None),
            P(),
            P(None, TP),
            P(None, TP),
            P(None, TP),
            P(None, TP),
            P(TP, None),
            P(),
        ),
        out_specs=P(whole, None),
        check_vma=False,
    )
```

```python
import jax
import jax.numpy as jnp
from jax import lax
from jax.experimental import pallas as pl
from jax.experimental.pallas import tpu as pltpu
from jax.sharding import Mesh
from jax.sharding import PartitionSpec as P

D = 2048
HEAD = 256
KV_HEADS = 2
CONV = 3
TGT_DEV = 128
PAD = 16
EPS = 1e-06

SP = ("zq", "zm", "ym", "yq")
TP = ("g", "xp", "c")
CHIPS = ("g", "xp")
SLICES = ("zm", "ym")
SAME_SLICE = ("yq", "zq")
BLOCK = 16
HALF = TGT_DEV // 2
bf16 = jnp.bfloat16
f32 = jnp.float32


def normalize(values, gain):
    widened = values.astype(f32)
    scaled = widened * lax.rsqrt(jnp.mean(widened * widened, axis=-1, keepdims=True) + EPS)
    return (scaled * gain).astype(bf16)


def attend_body(q_ref, own_ref, other_ref, o_ref):
    sources = (own_ref, other_ref)
    row = lax.broadcasted_iota(jnp.int32, (PAD, HEAD), 0)
    for at in range(0, q_ref.shape[0], 4):
        q = q_ref[at : at + 4].reshape(4 * HALF, HEAD)
        scores = [
            lax.dot_general(
                q, kv[:, :HEAD], (((1,), (1,)), ((), ())), preferred_element_type=f32
            )
            for kv in sources
        ]
        tops = [jnp.max(s, axis=1, keepdims=True) for s in scores]
        top = jnp.maximum(tops[0], tops[1])
        probs = [jnp.exp(s - top) for s in scores]
        total = sum(jnp.sum(p, axis=1, keepdims=True) for p in probs)
        o = sum(
            jnp.dot(p.astype(bf16), kv[:, HEAD:], preferred_element_type=f32)
            for p, kv in zip(probs, sources)
        )
        o = (o / total).astype(bf16)
        lse = top + jnp.log(total)
        for b in range(2):
            o_ref[at // 2 + b, :TGT_DEV, :] = o[b * TGT_DEV : (b + 1) * TGT_DEV]
            column = lse[b * TGT_DEV : (b + 1) * TGT_DEV]
            line = jnp.broadcast_to(column, (TGT_DEV, TGT_DEV)).T[:1]
            hi = line.astype(bf16).astype(f32)
            mid = (line - hi).astype(bf16).astype(f32)
            lo = line - hi - mid
            first = jnp.concatenate([hi, mid], axis=1)
            second = jnp.concatenate([lo, jnp.zeros_like(lo)], axis=1)
            tile = jnp.where(row == 0, first, jnp.where(row == 1, second, 0.0))
            o_ref[at // 2 + b, TGT_DEV:, :] = tile.astype(bf16)


def attend(queries, own, other, step=8):
    blocks = queries.shape[0]
    return pl.pallas_call(
        attend_body,
        grid=(blocks // step,),
        in_specs=[
            pl.BlockSpec((step, HALF, HEAD), lambda i: (i, 0, 0)),
            pl.BlockSpec(own.shape, lambda i: (0, 0)),
            pl.BlockSpec(memory_space=pltpu.VMEM),
        ],
        out_specs=pl.BlockSpec((step // 2, TGT_DEV + PAD, HEAD), lambda i: (i, 0, 0)),
        out_shape=pltpu.VMEM((blocks // 2, TGT_DEV + PAD, HEAD), bf16),
    )(queries, own, in_vmem(other))


def merge_body(parts_ref, own_hbm, other_hbm, o_ref, held, sem):
    copies = [
        pltpu.make_async_copy(w, held.at[k], sem.at[k]) for k, w in enumerate((own_hbm, other_hbm))
    ]
    for copy in copies:
        copy.start()
    count = parts_ref.shape[0]
    tail = parts_ref[:, TGT_DEV:, :].astype(f32)
    lse = tail[:, 0, :TGT_DEV] + tail[:, 0, TGT_DEV:] + tail[:, 1, :TGT_DEV]
    weight = jnp.exp(lse - jnp.max(lse, axis=0, keepdims=True))
    weight = (weight / jnp.sum(weight, axis=0, keepdims=True)).T
    merged = parts_ref[0, :TGT_DEV, :].astype(f32) * weight[:, :1]
    for t in range(1, count):
        merged = merged + parts_ref[t, :TGT_DEV, :].astype(f32) * weight[:, t : t + 1]
    merged = merged.astype(bf16)
    copies[0].wait()
    projected = jnp.dot(merged[:HALF], held[0], preferred_element_type=f32)
    copies[1].wait()
    projected += jnp.dot(merged[HALF:], held[1], preferred_element_type=f32)
    projected = projected.astype(bf16)
    for t in range(o_ref.shape[0]):
        o_ref[t] = projected


def in_vmem(array):
    return pltpu.with_memory_space_constraint(array, pltpu.VMEM)


def merge_project(parts, own, other, copies):
    hbm = pl.BlockSpec(memory_space=pl.ANY)
    return pl.pallas_call(
        merge_body,
        in_specs=[pl.BlockSpec(memory_space=pltpu.VMEM), hbm, hbm],
        out_shape=jax.ShapeDtypeStruct((copies, HALF, D), bf16),
        scratch_shapes=[pltpu.VMEM((2, *own.shape), bf16), pltpu.SemaphoreType.DMA((2,))],
    )(in_vmem(parts), own, other)


def mixer_in_body(tiles_ref, target_hbm, gain_ref, *refs):
    weights, (res_ref, gu_ref, tails_ref, last_ref) = refs[:4], refs[4:8]
    target_ref, held, sem = refs[8:]
    arrive = pltpu.make_async_copy(target_hbm, target_ref, sem.at[4])
    arrive.start()
    copies = [pltpu.make_async_copy(w, held.at[k], sem.at[k]) for k, w in enumerate(weights)]
    for copy in copies:
        copy.start()
    arrive.wait()
    projected = tiles_ref[0].astype(f32)
    for t in range(1, tiles_ref.shape[0]):
        projected = projected + tiles_ref[t].astype(f32)
    residual = (target_ref[...].astype(f32) + projected).astype(bf16)
    res_ref[...] = residual
    rows = normalize(residual, gain_ref[...])
    width = held.shape[2]
    for k, copy in enumerate(copies):
        copy.wait()
        part = jnp.dot(rows, held[k], preferred_element_type=f32).astype(bf16)
        gu_ref[:, k * width : (k + 1) * width] = part
        last = [part[b + BLOCK - (CONV - 1) : b + BLOCK] for b in range(0, HALF, BLOCK)]
        tails_ref[:, k * width : (k + 1) * width] = jnp.concatenate(last, axis=0)
        last_ref[:, k * width : (k + 1) * width] = last[-1]


def mixer_in(tiles, target, gain, weights):
    vmem = pl.BlockSpec(memory_space=pltpu.VMEM)
    hbm = pl.BlockSpec(memory_space=pl.ANY)
    width = weights[0].shape[1]
    count = len(weights)
    return pl.pallas_call(
        mixer_in_body,
        in_specs=[vmem, hbm, vmem] + [hbm] * count,
        out_shape=[
            pltpu.VMEM((HALF, D), bf16),
            pltpu.VMEM((HALF, count * width), bf16),
            pltpu.VMEM((HALF // BLOCK * (CONV - 1), count * width), bf16),
            pltpu.VMEM((CONV - 1, count * width), bf16),
        ],
        scratch_shapes=[
            pltpu.VMEM(target.shape, bf16),
            pltpu.VMEM((count, D, width), bf16),
            pltpu.SemaphoreType.DMA((count + 1,)),
        ],
    )(in_vmem(tiles), target, gain.reshape(1, D), *weights)


def mixer_out_body(core_ref, gu_ref, across_ref, before_ref, taps_ref, down_ref, other_ref, o_ref, held, sem):
    copies = [
        pltpu.make_async_copy(w, held.at[k], sem.at[k]) for k, w in enumerate((down_ref, other_ref))
    ]
    for copy in copies:
        copy.start()
    width = held.shape[1]
    halo = CONV - 1
    first = core_ref[0] == 0
    across = across_ref[...].astype(f32)
    before = before_ref[...].astype(f32)
    shifted = jnp.concatenate([before, across[:-halo]], axis=0)
    earlier = jnp.where(first, shifted, across)

    place = lax.broadcasted_iota(jnp.int32, (HALF, width), 0) % BLOCK

    def spread(row, from_at):
        return jnp.concatenate(
            [
                jnp.broadcast_to(
                    earlier[b * halo + row : b * halo + row + 1, from_at : from_at + width],
                    (BLOCK, width),
                )
                for b in range(HALF // BLOCK)
            ],
            axis=0,
        )

    def convolved(at, from_at, tap_row, tap_at):
        here = gu_ref[:, at : at + width].astype(f32)
        last = spread(1, from_at)
        one = jnp.where(place == 0, last, pltpu.roll(here, 1, 0))
        two = jnp.where(place == 1, last, pltpu.roll(here, 2, 0))
        two = jnp.where(place == 0, spread(0, from_at), two)
        scale = taps_ref[tap_row : tap_row + CONV, tap_at : tap_at + width]
        return scale[0:1] * two + scale[1:2] * one + scale[2:3] * here

    total = 0.0
    for k, copy in enumerate(copies):
        gate = convolved(k * width, (1 - k) * width, 0, k * width)
        up = convolved((2 + k) * width, (3 - k) * width, CONV, k * width)
        hidden = (gate / (1.0 + jnp.exp(-gate)) * up).astype(bf16)
        copy.wait()
        total = total + jnp.dot(hidden, held[k], preferred_element_type=f32)
    o_ref[...] = total.astype(bf16)


def mixer_out(core, gate_up, across, before, taps, down, other):
    vmem = pl.BlockSpec(memory_space=pltpu.VMEM)
    hbm = pl.BlockSpec(memory_space=pl.ANY)
    return pl.pallas_call(
        mixer_out_body,
        in_specs=[pl.BlockSpec(memory_space=pltpu.SMEM), vmem, vmem, vmem, vmem, hbm, hbm],
        out_shape=pltpu.VMEM((HALF, D), bf16),
        scratch_shapes=[pltpu.VMEM((2, *down.shape), bf16), pltpu.SemaphoreType.DMA((2,))],
    )(core, in_vmem(gate_up), in_vmem(across), in_vmem(before), taps, down, other)


def exchanged(array, axes):
    return lax.all_to_all(array, axes, 0, 0, tiled=True)


def sent_to_all(shard, axes):
    count = lax.axis_size(axes)
    return exchanged(jnp.broadcast_to(shard, (count, *shard.shape)), axes)


def other_core(array):
    return lax.ppermute(array, "c", [(0, 1), (1, 0)])


def from_last_line(array):
    lines = lax.axis_size(SP)
    axes = (*SP, "c")
    return lax.ppermute(array, axes, [(2 * i + 1, 2 * i + 2) for i in range(lines - 1)])


def shards(
    target,
    source,
    query_gain,
    source_gain,
    query_weight,
    key_weight,
    value_weight,
    out_weight,
    mixer_gain,
    gate_weight,
    up_weight,
    gate_taps,
    up_taps,
    down_weight,
    final_gain,
):
    core = lax.axis_index("c")
    chip = lax.axis_index(CHIPS)
    source_normed = normalize(source, source_gain)
    key_rows = jnp.dot(source_normed, key_weight, preferred_element_type=f32).astype(bf16)
    value_rows = jnp.dot(source_normed, value_weight, preferred_element_type=f32).astype(bf16)
    rows = source.shape[0]
    by_head = jnp.stack(
        [
            jnp.concatenate([key_rows[:, :HEAD], value_rows[:, :HEAD]], axis=1),
            jnp.concatenate([key_rows[:, HEAD:], value_rows[:, HEAD:]], axis=1),
        ]
    )
    near_lines = lax.axis_size(SAME_SLICE)
    by_head = by_head.reshape(KV_HEADS * rows, 2 * HEAD)
    near = sent_to_all(by_head, SAME_SLICE)
    near = near.reshape(near_lines, KV_HEADS, rows, 2 * HEAD).transpose(1, 0, 2, 3)
    near = near.reshape(KV_HEADS, 1, near_lines * rows, 2 * HEAD)
    chips = lax.axis_size(CHIPS)
    near = jnp.broadcast_to(near, (KV_HEADS, chips // KV_HEADS, *near.shape[2:]))
    kv = exchanged(near.reshape(chips, *near.shape[2:]), CHIPS).reshape(-1, 2 * HEAD)

    normed = normalize(target, query_gain)
    own_query = jnp.dot(normed, query_weight, preferred_element_type=f32).astype(bf16)
    own_query = own_query * jnp.asarray(HEAD ** (-0.5), bf16)
    by_core = own_query.reshape(4, 2, BLOCK, HEAD)
    kept = lax.dynamic_index_in_dim(by_core, core, 1, False).reshape(HALF, HEAD)
    given = lax.dynamic_index_in_dim(by_core, 1 - core, 1, False).reshape(HALF, HEAD)
    given = other_core(given)
    both = jnp.stack([kept, given])
    queries = lax.all_gather(both[None], "ym", axis=0, tiled=True)
    queries = lax.all_gather(queries[None], "zm", axis=0, tiled=True)
    queries = queries.reshape(-1, HALF, HEAD)
    target_half = lax.dynamic_index_in_dim(target.reshape(4, 2, BLOCK, D), core, 1, False)
    target_half = target_half.reshape(HALF, D)
    queries, target_half = lax.optimization_barrier((queries, target_half))
    attended = attend(queries, kv, other_core(kv))
    parts = exchanged(attended, SLICES)
    out_other = other_core(out_weight)
    gate_other = other_core(gate_weight)
    up_other = other_core(up_weight)
    down_other = other_core(down_weight)
    taps = jnp.concatenate([gate_taps, up_taps], axis=0)
    taps_other = other_core(taps)
    taps = jnp.concatenate([taps, taps_other], axis=1).astype(f32)
    core_at = core.astype(jnp.int32).reshape(1)
    partial = merge_project(parts, out_weight, out_other, chips)
    residual, gate_up, tails, last = mixer_in(
        exchanged(partial, CHIPS),
        target_half,
        mixer_gain,
        (gate_weight, gate_other, up_weight, up_other),
    )
    before = from_last_line(last)
    across = other_core(tails)
    partial = mixer_out(core_at, gate_up, across, before, taps, down_weight, down_other)
    tiles = exchanged(partial.reshape(HALF // BLOCK, BLOCK, D), CHIPS)
    mixer = jnp.sum(tiles.astype(f32), axis=0)
    own_rows = lax.dynamic_slice_in_dim(residual, chip * BLOCK, BLOCK, 0)
    return normalize(own_rows.astype(f32) + mixer, final_gain)


def solution(mesh):
    lines = mesh.shape["sp"]
    devices = mesh.devices.reshape(lines // 32, 4, 2, 4, 2, 2, 2)
    split = Mesh(devices, SP + TP)
    whole = SP + TP
    return jax.shard_map(
        shards,
        mesh=split,
        in_specs=(
            P(SP, None),
            P(whole, None),
            P(),
            P(),
            P(None, TP),
            P(),
            P(),
            P(TP, None),
            P(),
            P(None, TP),
            P(None, TP),
            P(None, TP),
            P(None, TP),
            P(TP, None),
            P(),
        ),
        out_specs=P(whole, None),
        check_vma=False,
    )
```

```python
import jax
import jax.numpy as jnp
from jax import lax
from jax.experimental import pallas as pl
from jax.experimental.pallas import tpu as pltpu
from jax.sharding import Mesh
from jax.sharding import PartitionSpec as P

D = 2048
HEAD = 256
KV_HEADS = 2
CONV = 3
TGT_DEV = 128
PAD = 16
EPS = 1e-06

SP = ("zq", "zm", "ym", "yq")
TP = ("g", "xp", "c")
CHIPS = ("g", "xp")
SLICES = ("zm", "ym")
SAME_SLICE = ("yq", "zq")
BLOCK = 16
HALF = TGT_DEV // 2
bf16 = jnp.bfloat16
f32 = jnp.float32


def normalize(values, gain):
    widened = values.astype(f32)
    scaled = widened * lax.rsqrt(jnp.mean(widened * widened, axis=-1, keepdims=True) + EPS)
    return (scaled * gain).astype(bf16)


def source_body(source_hbm, gain_hbm, key_hbm, value_hbm, o_ref, source_ref, gain_ref, held, sem):
    arrive = [
        pltpu.make_async_copy(source_hbm, source_ref, sem.at[2]),
        pltpu.make_async_copy(gain_hbm, gain_ref, sem.at[3]),
    ]
    copies = [
        pltpu.make_async_copy(w, held.at[k], sem.at[k]) for k, w in enumerate((key_hbm, value_hbm))
    ]
    for copy in arrive + copies:
        copy.start()
    for copy in arrive:
        copy.wait()
    rows = normalize(source_ref[...], gain_ref[...])
    parts = []
    for k, copy in enumerate(copies):
        copy.wait()
        parts.append(jnp.dot(rows, held[k], preferred_element_type=f32).astype(bf16))
    by_head = [
        jnp.concatenate([part[:, h * HEAD : (h + 1) * HEAD] for part in parts], axis=1)
        for h in range(KV_HEADS)
    ]
    by_head = jnp.concatenate(by_head, axis=0)
    for t in range(o_ref.shape[0]):
        o_ref[t] = by_head


def project_source(source, gain, key_weight, value_weight, copies):
    rows = source.shape[0]
    return pl.pallas_call(
        source_body,
        in_specs=[pl.BlockSpec(memory_space=pl.ANY)] * 4,
        out_shape=jax.ShapeDtypeStruct((copies, KV_HEADS * rows, 2 * HEAD), bf16),
        scratch_shapes=[
            pltpu.VMEM(source.shape, bf16),
            pltpu.VMEM((1, D), f32),
            pltpu.VMEM((2, *key_weight.shape), bf16),
            pltpu.SemaphoreType.DMA((4,)),
        ],
    )(source, gain.reshape(1, D), key_weight, value_weight)


def attend_body(q_ref, own_ref, other_ref, o_ref):
    sources = (own_ref, other_ref)
    row = lax.broadcasted_iota(jnp.int32, (PAD, HEAD), 0)
    for at in range(0, q_ref.shape[0], 4):
        q = q_ref[at : at + 4].reshape(4 * HALF, HEAD)
        scores = [
            lax.dot_general(
                q, kv[:, :HEAD], (((1,), (1,)), ((), ())), preferred_element_type=f32
            )
            for kv in sources
        ]
        tops = [jnp.max(s, axis=1, keepdims=True) for s in scores]
        top = jnp.maximum(tops[0], tops[1])
        probs = [jnp.exp(s - top) for s in scores]
        total = sum(jnp.sum(p, axis=1, keepdims=True) for p in probs)
        o = sum(
            jnp.dot(p.astype(bf16), kv[:, HEAD:], preferred_element_type=f32)
            for p, kv in zip(probs, sources)
        )
        o = (o / total).astype(bf16)
        lse = top + jnp.log(total)
        for b in range(2):
            o_ref[at // 2 + b, :TGT_DEV, :] = o[b * TGT_DEV : (b + 1) * TGT_DEV]
            column = lse[b * TGT_DEV : (b + 1) * TGT_DEV]
            line = jnp.broadcast_to(column, (TGT_DEV, TGT_DEV)).T[:1]
            hi = line.astype(bf16).astype(f32)
            mid = (line - hi).astype(bf16).astype(f32)
            lo = line - hi - mid
            first = jnp.concatenate([hi, mid], axis=1)
            second = jnp.concatenate([lo, jnp.zeros_like(lo)], axis=1)
            tile = jnp.where(row == 0, first, jnp.where(row == 1, second, 0.0))
            o_ref[at // 2 + b, TGT_DEV:, :] = tile.astype(bf16)


def attend(queries, own, other, step=8):
    blocks = queries.shape[0]
    return pl.pallas_call(
        attend_body,
        grid=(blocks // step,),
        in_specs=[
            pl.BlockSpec((step, HALF, HEAD), lambda i: (i, 0, 0)),
            pl.BlockSpec(memory_space=pltpu.VMEM),
            pl.BlockSpec(other.shape, lambda i: (0, 0)),
        ],
        out_specs=pl.BlockSpec((step // 2, TGT_DEV + PAD, HEAD), lambda i: (i, 0, 0)),
        out_shape=pltpu.VMEM((blocks // 2, TGT_DEV + PAD, HEAD), bf16),
    )(queries, in_vmem(own), other)


def merge_body(parts_ref, own_hbm, other_hbm, o_ref, held, sem):
    copies = [
        pltpu.make_async_copy(w, held.at[k], sem.at[k]) for k, w in enumerate((own_hbm, other_hbm))
    ]
    for copy in copies:
        copy.start()
    count = parts_ref.shape[0]
    tail = parts_ref[:, TGT_DEV:, :].astype(f32)
    lse = tail[:, 0, :TGT_DEV] + tail[:, 0, TGT_DEV:] + tail[:, 1, :TGT_DEV]
    weight = jnp.exp(lse - jnp.max(lse, axis=0, keepdims=True))
    weight = (weight / jnp.sum(weight, axis=0, keepdims=True)).T
    merged = parts_ref[0, :TGT_DEV, :].astype(f32) * weight[:, :1]
    for t in range(1, count):
        merged = merged + parts_ref[t, :TGT_DEV, :].astype(f32) * weight[:, t : t + 1]
    merged = merged.astype(bf16)
    copies[0].wait()
    projected = jnp.dot(merged[:HALF], held[0], preferred_element_type=f32)
    copies[1].wait()
    projected += jnp.dot(merged[HALF:], held[1], preferred_element_type=f32)
    projected = projected.astype(bf16)
    for t in range(o_ref.shape[0]):
        o_ref[t] = projected


def in_vmem(array):
    return pltpu.with_memory_space_constraint(array, pltpu.VMEM)


def merge_project(parts, own, other, copies):
    hbm = pl.BlockSpec(memory_space=pl.ANY)
    return pl.pallas_call(
        merge_body,
        in_specs=[pl.BlockSpec(memory_space=pltpu.VMEM), hbm, hbm],
        out_shape=jax.ShapeDtypeStruct((copies, HALF, D), bf16),
        scratch_shapes=[pltpu.VMEM((2, *own.shape), bf16), pltpu.SemaphoreType.DMA((2,))],
    )(in_vmem(parts), own, other)


def mixer_in_body(tiles_ref, target_hbm, gain_ref, *refs):
    weights, (res_ref, gu_ref, tails_ref, last_ref) = refs[:4], refs[4:8]
    target_ref, held, sem = refs[8:]
    arrive = pltpu.make_async_copy(target_hbm, target_ref, sem.at[4])
    arrive.start()
    copies = [pltpu.make_async_copy(w, held.at[k], sem.at[k]) for k, w in enumerate(weights)]
    for copy in copies:
        copy.start()
    arrive.wait()
    projected = tiles_ref[0].astype(f32)
    for t in range(1, tiles_ref.shape[0]):
        projected = projected + tiles_ref[t].astype(f32)
    residual = (target_ref[...].astype(f32) + projected).astype(bf16)
    res_ref[...] = residual
    rows = normalize(residual, gain_ref[...])
    width = held.shape[2]
    for k, copy in enumerate(copies):
        copy.wait()
        part = jnp.dot(rows, held[k], preferred_element_type=f32).astype(bf16)
        gu_ref[:, k * width : (k + 1) * width] = part
        last = [part[b + BLOCK - (CONV - 1) : b + BLOCK] for b in range(0, HALF, BLOCK)]
        tails_ref[:, k * width : (k + 1) * width] = jnp.concatenate(last, axis=0)
        last_ref[:, k * width : (k + 1) * width] = last[-1]


def mixer_in(tiles, target, gain, weights):
    vmem = pl.BlockSpec(memory_space=pltpu.VMEM)
    hbm = pl.BlockSpec(memory_space=pl.ANY)
    width = weights[0].shape[1]
    count = len(weights)
    return pl.pallas_call(
        mixer_in_body,
        in_specs=[vmem, hbm, vmem] + [hbm] * count,
        out_shape=[
            pltpu.VMEM((HALF, D), bf16),
            pltpu.VMEM((HALF, count * width), bf16),
            pltpu.VMEM((HALF // BLOCK * (CONV - 1), count * width), bf16),
            pltpu.VMEM((CONV - 1, count * width), bf16),
        ],
        scratch_shapes=[
            pltpu.VMEM(target.shape, bf16),
            pltpu.VMEM((count, D, width), bf16),
            pltpu.SemaphoreType.DMA((count + 1,)),
        ],
    )(in_vmem(tiles), target, gain.reshape(1, D), *weights)


def mixer_out_body(
    core_ref, gu_ref, across_ref, before_ref, taps_hbm, down_ref, other_ref, o_ref, held, taps_ref, sem
):
    copies = [
        pltpu.make_async_copy(w, held.at[k], sem.at[k]) for k, w in enumerate((down_ref, other_ref))
    ]
    for copy in copies:
        copy.start()
    taps_copy = pltpu.make_async_copy(taps_hbm, taps_ref, sem.at[2])
    taps_copy.start()
    width = held.shape[1]
    halo = CONV - 1
    first = core_ref[0] == 0
    across = across_ref[...].astype(f32)
    before = before_ref[...].astype(f32)
    shifted = jnp.concatenate([before, across[:-halo]], axis=0)
    earlier = jnp.where(first, shifted, across)

    place = lax.broadcasted_iota(jnp.int32, (HALF, width), 0) % BLOCK

    def spread(row, from_at):
        return jnp.concatenate(
            [
                jnp.broadcast_to(
                    earlier[b * halo + row : b * halo + row + 1, from_at : from_at + width],
                    (BLOCK, width),
                )
                for b in range(HALF // BLOCK)
            ],
            axis=0,
        )

    def convolved(at, from_at, tap_row, tap_at):
        here = gu_ref[:, at : at + width].astype(f32)
        last = spread(1, from_at)
        one = jnp.where(place == 0, last, pltpu.roll(here, 1, 0))
        two = jnp.where(place == 1, last, pltpu.roll(here, 2, 0))
        two = jnp.where(place == 0, spread(0, from_at), two)
        scale = taps_ref[tap_row : tap_row + CONV, tap_at : tap_at + width]
        return scale[0:1] * two + scale[1:2] * one + scale[2:3] * here

    taps_copy.wait()
    total = 0.0
    for k, copy in enumerate(copies):
        gate = convolved(k * width, (1 - k) * width, 0, k * width)
        up = convolved((2 + k) * width, (3 - k) * width, CONV, k * width)
        hidden = (gate / (1.0 + jnp.exp(-gate)) * up).astype(bf16)
        copy.wait()
        total = total + jnp.dot(hidden, held[k], preferred_element_type=f32)
    o_ref[...] = total.astype(bf16)


def mixer_out(core, gate_up, across, before, taps, down, other):
    vmem = pl.BlockSpec(memory_space=pltpu.VMEM)
    hbm = pl.BlockSpec(memory_space=pl.ANY)
    return pl.pallas_call(
        mixer_out_body,
        in_specs=[pl.BlockSpec(memory_space=pltpu.SMEM), vmem, vmem, vmem, hbm, hbm, hbm],
        out_shape=pltpu.VMEM((HALF, D), bf16),
        scratch_shapes=[
            pltpu.VMEM((2, *down.shape), bf16),
            pltpu.VMEM(taps.shape, f32),
            pltpu.SemaphoreType.DMA((3,)),
        ],
    )(core, in_vmem(gate_up), in_vmem(across), in_vmem(before), taps, down, other)


def exchanged(array, axes):
    return lax.all_to_all(array, axes, 0, 0, tiled=True)


def other_core(array):
    return lax.ppermute(array, "c", [(0, 1), (1, 0)])


def from_last_line(array):
    lines = lax.axis_size(SP)
    axes = (*SP, "c")
    return lax.ppermute(array, axes, [(2 * i + 1, 2 * i + 2) for i in range(lines - 1)])


def shards(
    target,
    source,
    query_gain,
    source_gain,
    query_weight,
    key_weight,
    value_weight,
    out_weight,
    mixer_gain,
    gate_weight,
    up_weight,
    gate_taps,
    up_taps,
    down_weight,
    final_gain,
):
    core = lax.axis_index("c")
    chip = lax.axis_index(CHIPS)
    rows = source.shape[0]
    near_lines = lax.axis_size(SAME_SLICE)
    near = project_source(source, source_gain, key_weight, value_weight, near_lines)
    near = exchanged(near, SAME_SLICE)
    near = near.reshape(near_lines, KV_HEADS, rows, 2 * HEAD).transpose(1, 0, 2, 3)
    near = near.reshape(KV_HEADS, 1, near_lines * rows, 2 * HEAD)
    chips = lax.axis_size(CHIPS)
    near = jnp.broadcast_to(near, (KV_HEADS, chips // KV_HEADS, *near.shape[2:]))
    kv = exchanged(near.reshape(chips, *near.shape[2:]), CHIPS).reshape(-1, 2 * HEAD)

    normed = normalize(target, query_gain)
    own_query = jnp.dot(normed, query_weight, preferred_element_type=f32).astype(bf16)
    own_query = own_query * jnp.asarray(HEAD ** (-0.5), bf16)
    by_core = own_query.reshape(4, 2, BLOCK, HEAD)
    kept = lax.dynamic_index_in_dim(by_core, core, 1, False).reshape(HALF, HEAD)
    given = lax.dynamic_index_in_dim(by_core, 1 - core, 1, False).reshape(HALF, HEAD)
    given = other_core(given)
    both = jnp.stack([kept, given])
    queries = lax.all_gather(both[None], "ym", axis=0, tiled=True)
    queries = lax.all_gather(queries[None], "zm", axis=0, tiled=True)
    queries = queries.reshape(-1, HALF, HEAD)
    target_half = lax.dynamic_index_in_dim(target.reshape(4, 2, BLOCK, D), core, 1, False)
    target_half = target_half.reshape(HALF, D)
    queries, target_half = lax.optimization_barrier((queries, target_half))
    attended = attend(queries, kv, other_core(kv))
    parts = exchanged(attended, SLICES)
    gate_other = other_core(gate_weight)
    up_other = other_core(up_weight)
    down_other = other_core(down_weight)
    out_other = other_core(out_weight)
    taps = jnp.concatenate([gate_taps, up_taps], axis=0)
    taps_other = other_core(taps)
    taps = jnp.concatenate([taps, taps_other], axis=1).astype(f32)
    core_at = core.astype(jnp.int32).reshape(1)
    partial = merge_project(parts, out_weight, out_other, chips)
    residual, gate_up, tails, last = mixer_in(
        exchanged(partial, CHIPS),
        target_half,
        mixer_gain,
        (gate_weight, gate_other, up_weight, up_other),
    )
    before = from_last_line(last)
    across = other_core(tails)
    partial = mixer_out(core_at, gate_up, across, before, taps, down_weight, down_other)
    tiles = exchanged(partial.reshape(HALF // BLOCK, BLOCK, D), CHIPS)
    mixer = jnp.sum(tiles.astype(f32), axis=0)
    own_rows = lax.dynamic_slice_in_dim(residual, chip * BLOCK, BLOCK, 0)
    return normalize(own_rows.astype(f32) + mixer, final_gain)


def solution(mesh):
    lines = mesh.shape["sp"]
    devices = mesh.devices.reshape(lines // 32, 4, 2, 4, 2, 2, 2)
    split = Mesh(devices, SP + TP)
    whole = SP + TP
    return jax.shard_map(
        shards,
        mesh=split,
        in_specs=(
            P(SP, None),
            P(whole, None),
            P(),
            P(),
            P(None, TP),
            P(),
            P(),
            P(TP, None),
            P(),
            P(None, TP),
            P(None, TP),
            P(None, TP),
            P(None, TP),
            P(TP, None),
            P(),
        ),
        out_specs=P(whole, None),
        check_vma=False,
    )
```
